32 devices in a mesh: dp: 4 (over y, x), kv: 4 (over z), tp: 2 (over core).
Axes of the slice: x: 2, y: 2, z: 4, core: 2. Of those that a mesh axis runs over, the one named last changes fastest.
Arguments:
- tokens: bfloat16 [32, 4096], P('dp', ('kv', 'tp')), as said below
- query_weight: bfloat16 [4096, 16, 128], P(None, 'tp', 'kv'), may hold values from -0.09375 to 0.09375
- key_weight: bfloat16 [4096, 16, 128], P(None, 'tp', 'kv'), may hold values from -0.09375 to 0.09375
- value_weight: bfloat16 [4096, 16, 256], P(None, 'tp', 'kv'), may hold values from -0.09375 to 0.09375
- gate_weight: bfloat16 [4096, 16, 256], P(None, 'tp', 'kv'), may hold values from -0.09375 to 0.09375
- decay_weight: bfloat16 [4096, 16, 128], P(None, 'tp', 'kv'), may hold values from -0.09375 to 0.09375
- decay_bias: float32 [16, 128], P('tp'), may hold values from -8 to 2
- states: float32 [32, 16, 128, 256], P(('dp', 'kv'), 'tp'), may hold values from -4 to 4
- head_gain: float32 [16, 256], P('tp'), may hold values from 0.1 to 1.9
- out_weight: bfloat16 [4096, 4096], P(None, ('kv', 'tp')), as said below
- norm1_gain: float32 [4096], P(('kv', 'tp')), may hold values from 0.1 to 1.9
- norm1_bias: float32 [4096], P(('kv', 'tp')), may hold values from -3 to 3
- up_weight: bfloat16 [4096, 16384], P(None, ('kv', 'tp')), may hold values from -0.09375 to 0.09375
- down_weight: bfloat16 [16384, 4096], P(('kv', 'tp')), as said below
- norm2_gain: float32 [4096], P(('kv', 'tp')), may hold values from 0.1 to 1.9
- norm2_bias: float32 [4096], P(('kv', 'tp')), may hold values from -3 to 3
Outputs:
- layer_out: bfloat16 [32, 4096], P('dp', ('kv', 'tp'))
- new_states: float32 [32, 16, 128, 256], P(('dp', 'kv'), 'tp')
The draws below stay inside these ranges and needn't reach their ends.
Inputs may be any that keep to these rules, and one draw needn't show every extreme that they name: `tokens`: each block of 64 features has its own scale. `out_weight`: entries lie within 13 / sqrt(4096) of zero. `down_weight`: entries lie within 14 / sqrt(16384) of zero.
All inputs are finite; a program needn't handle non-finite values.
Results may differ from the reference program's by a relative error of at most 0.009.
Values may be sent and summed in bfloat16 or wider, within the bound.
No kernel may reach another device: no remote copies, remote signals or barrier semaphores. Data moves between devices by JAX's collectives and lax.ppermute only.
A program may use at most 128 MiB of HBM per device.

```python
import jax
import jax.numpy as jnp
from jax import lax

D = 4096
HEADS = 16
KEY_DIM = 128
VALUE_DIM = 256
MIXER_UNITS = 16384
ROWS = 32


def draw_tokens(key, part):
    base_key, scale_key = jax.random.split(key, 2)
    column_scale = jnp.exp(jax.random.uniform(scale_key, (D // 64,), jnp.float32, -1.0, 1.0))
    column_scale = jnp.repeat(column_scale, 64)
    values = jax.random.normal(base_key, (ROWS, D), jnp.float32)
    return (values * column_scale).astype(jnp.bfloat16)


def draw_out_weight(key, part):
    noise_key, left_key, right_key = jax.random.split(jax.random.fold_in(key, 31), 3)
    fan_in = HEADS * VALUE_DIM
    left = jnp.clip(jax.random.normal(left_key, (fan_in, 1), jnp.float32), -3.0, 3.0)
    right = jnp.clip(jax.random.normal(right_key, (1, D), jnp.float32), -3.0, 3.0)
    noise = jnp.clip(jax.random.normal(noise_key, (fan_in, D), jnp.float32), -6.0, 6.0)
    common = 0.8 * left * right
    return ((0.6 * noise + common) * fan_in ** (-0.5)).astype(jnp.bfloat16)


def draw_down_weight(key, part):
    noise_key, offset_key = jax.random.split(jax.random.fold_in(key, 47), 2)
    noise = jnp.clip(jax.random.normal(noise_key, (MIXER_UNITS, D), jnp.float32), -6.0, 6.0)
    offset = jax.random.uniform(offset_key, (1, D), jnp.float32, -5.0, 5.0)
    values = noise * MIXER_UNITS ** (-0.5) + offset / MIXER_UNITS
    return values.astype(jnp.bfloat16)


def block_levels(own_key, dims, shards, low, top_value):
    level, own = 1.0, jax.random.fold_in(own_key, 6)
    for dim, blocks in shards:
        steps = jnp.exp(jax.random.uniform(jax.random.fold_in(own, dim), (blocks,), jnp.float32, low / len(shards), top_value / len(shards)))
        level = level * jnp.repeat(steps, dims[dim] // blocks).reshape([-1 if axis == dim else 1 for axis in range(len(dims))])
    return level


def scatter_about(stream_key, shape, scale, reach, cuts=(), kind=jnp.bfloat16):
    values = scale * jax.random.normal(stream_key, shape, jnp.float32)
    if cuts:
        values = values * block_levels(stream_key, shape, cuts, -0.22, 0.18)
    return jnp.clip(values, -reach, reach).astype(kind)


def setup_inputs(seed: int = 0) -> dict:
    keys = jax.random.split(jax.random.key(seed), 17)
    return {
        "tokens": draw_tokens(jax.random.fold_in(keys[16], 71), 0),
        "query_weight": scatter_about(keys[1], (D, HEADS, KEY_DIM), D ** -0.5, 0.09375, ((1, 2), (2, 4))),
        "key_weight": scatter_about(keys[2], (D, HEADS, KEY_DIM), D ** -0.5, 0.09375, ((1, 2), (2, 4))),
        "value_weight": scatter_about(keys[3], (D, HEADS, VALUE_DIM), D ** -0.5, 0.09375, ((1, 2), (2, 4))),
        "gate_weight": scatter_about(keys[4], (D, HEADS, VALUE_DIM), D ** -0.5, 0.09375, ((1, 2), (2, 4))),
        "decay_weight": scatter_about(keys[5], (D, HEADS, KEY_DIM), D ** -0.5, 0.09375, ((1, 2), (2, 4))),
        "decay_bias": jnp.clip(-8.0 + 10.0 * jax.random.uniform(keys[6], (HEADS, KEY_DIM), jnp.float32) ** block_levels(keys[6], (HEADS, KEY_DIM), ((0, 2),), -0.2, 0.2), -8.0, 2.0),
        "states": scatter_about(keys[7], (ROWS, HEADS, KEY_DIM, VALUE_DIM), 0.5, 4.0, ((0, 16), (1, 2)), jnp.float32),
        "head_gain": jnp.clip(1.0 + 0.18 * jax.random.normal(keys[8], (HEADS, VALUE_DIM), jnp.float32), 0.1, 1.9),
        "out_weight": draw_out_weight(jax.random.fold_in(keys[16], 71), 0),
        "norm1_gain": jnp.clip(1.0 + 0.18 * jax.random.normal(keys[10], (D,), jnp.float32), 0.1, 1.9),
        "norm1_bias": scatter_about(keys[11], (D,), 0.5, 3.0, ((0, 8),), jnp.float32),
        "up_weight": scatter_about(keys[12], (D, MIXER_UNITS), D ** -0.5, 0.09375, ((1, 8),)),
        "down_weight": draw_down_weight(jax.random.fold_in(keys[16], 71), 0),
        "norm2_gain": jnp.clip(1.0 + 0.18 * jax.random.normal(keys[14], (D,), jnp.float32), 0.1, 1.9),
        "norm2_bias": scatter_about(keys[15], (D,), 0.5, 3.0, ((0, 8),), jnp.float32),
    }


ALPHA = 2.0 ** 0.5
TAU = 16.0
LN_EPS = 1e-05
RMS_EPS = 1e-06

def project(inputs, weight):
    flattened = weight.reshape(weight.shape[0], -1)
    return jnp.dot(inputs, flattened, preferred_element_type=jnp.float32).astype(jnp.bfloat16)

def normalize(inputs, row_gain, row_shift):
    average = lax.optimization_barrier(jnp.sum(inputs, axis=-1, keepdims=True)) / inputs.shape[-1]
    spread = lax.optimization_barrier(jnp.sum(inputs * inputs, axis=-1, keepdims=True)) / inputs.shape[-1] - average * average
    return ((inputs - average) * lax.rsqrt(spread + LN_EPS) * row_gain + row_shift).astype(jnp.bfloat16)

def reference(tokens, query_weight, key_weight, value_weight, gate_weight, decay_weight, decay_bias, states, head_gain, out_weight, norm1_gain, norm1_bias, up_weight, down_weight, norm2_gain, norm2_bias):
    row_count = tokens.shape[0]
    query_rows = project(tokens, query_weight).astype(jnp.float32).reshape(row_count, HEADS, KEY_DIM) * KEY_DIM ** (-0.5)
    key_rows = project(tokens, key_weight).astype(jnp.float32).reshape(row_count, HEADS, KEY_DIM)
    decay_rows = project(tokens, decay_weight).astype(jnp.float32).reshape(row_count, HEADS, KEY_DIM)
    value_rows = project(tokens, value_weight).astype(jnp.float32).reshape(row_count, HEADS, VALUE_DIM)
    gate_rows = project(tokens, gate_weight).astype(jnp.float32).reshape(row_count, HEADS, VALUE_DIM)
    retain = jnp.exp(jax.nn.log_sigmoid(decay_rows + decay_bias) / TAU)
    new_states = retain[..., None] * states + key_rows[..., :, None] * value_rows[..., None, :]
    readout = jnp.einsum('rhk,rhkv->rhv', query_rows, new_states, precision=lax.Precision.HIGHEST)
    readout = readout * lax.rsqrt(lax.optimization_barrier(jnp.mean(readout * readout, axis=-1, keepdims=True)) + RMS_EPS) * head_gain
    attended = (readout * jax.nn.silu(gate_rows)).astype(jnp.bfloat16).reshape(row_count, HEADS * VALUE_DIM)
    mixed_heads = jnp.dot(attended, out_weight, preferred_element_type=jnp.float32)
    residual_one = ALPHA * tokens.astype(jnp.float32) + mixed_heads
    normed = normalize(residual_one, norm1_gain, norm1_bias)
    lifted = jnp.dot(normed, up_weight, preferred_element_type=jnp.float32)
    hidden = jnp.square(jax.nn.relu(lifted)).astype(jnp.bfloat16)
    residual_two = ALPHA * normed.astype(jnp.float32) + jnp.dot(hidden, down_weight, preferred_element_type=jnp.float32)
    return (normalize(residual_two, norm2_gain, norm2_bias), new_states)
```

```python
import jax
import jax.numpy as jnp
from jax import lax
from jax.sharding import PartitionSpec as P

KEY_DIM = 128


ALPHA = 2.0**0.5
TAU = 16.0
LN_EPS = 1e-05
RMS_EPS = 1e-06


def project_flat(inputs, weight):
    flattened = weight.reshape(weight.shape[0], -1)
    return jnp.dot(inputs, flattened, preferred_element_type=jnp.float32).astype(jnp.bfloat16)


def normalize(inputs, average, spread, row_gain, row_shift):
    return ((inputs - average) * lax.rsqrt(spread + LN_EPS) * row_gain + row_shift).astype(
        jnp.bfloat16
    )

PEERS_MAX = 8


def exchanges(name):
    size = lax.axis_size(name)
    return size <= PEERS_MAX and size & (size - 1) == 0


def partner(value, name, step):
    size = lax.axis_size(name)
    return lax.ppermute(value, name, [(i, i ^ step) for i in range(size)])


def reorder(blocks, name):
    own = lax.axis_index(name)
    bit = 1
    while bit < len(blocks):
        flip = (own & bit) != 0
        blocks = [lax.select(flip, blocks[j ^ bit], blocks[j]) for j in range(len(blocks))]
        bit *= 2
    return blocks


def gather_blocks(value, name):
    size = lax.axis_size(name)
    if not exchanges(name):
        stacked = lax.all_gather(value, name)
        return [stacked[j] for j in range(size)]
    return reorder([value] + [partner(value, name, step) for step in range(1, size)], name)


def gather_columns(value):
    if not (exchanges("kv") and exchanges("tp")):
        return lax.all_gather(value, ("kv", "tp"), axis=1, tiled=True)
    pair = jnp.concatenate(gather_blocks(value, "tp"), axis=1)
    return jnp.concatenate(gather_blocks(pair, "kv"), axis=1)


def trade_rows(value, name):
    size = lax.axis_size(name)
    share = value.shape[0] // size
    if not exchanges(name):
        arrived = lax.all_to_all(value, name, split_axis=0, concat_axis=0, tiled=True)
        return [arrived[j * share : (j + 1) * share] for j in range(size)]
    outgoing = reorder([value[j * share : (j + 1) * share] for j in range(size)], name)
    arrived = outgoing[:1] + [partner(outgoing[step], name, step) for step in range(1, size)]
    return reorder(arrived, name)


def sums(values):
    return jnp.concatenate(
        [
            jnp.sum(values, axis=-1, keepdims=True),
            jnp.sum(values * values, axis=-1, keepdims=True),
        ],
        axis=-1,
    )


def moments(totals, width):
    average = totals[:, :1] / width
    return average, totals[:, 1:2] / width - average * average


def body(
    tokens,
    query_weight,
    key_weight,
    value_weight,
    gate_weight,
    decay_weight,
    decay_bias,
    states,
    head_gain,
    out_weight,
    norm1_gain,
    norm1_bias,
    up_weight,
    down_weight,
    norm2_gain,
    norm2_bias,
):
    whole = gather_columns(tokens)
    norm_rows = gather_columns(jnp.stack([norm1_gain, norm1_bias]))
    weights_list = (query_weight, key_weight, decay_weight, value_weight, gate_weight)
    packed = jnp.concatenate([project_flat(whole, weight) for weight in weights_list], axis=1)
    arrived = trade_rows(packed, "kv")
    groups = lax.axis_size("kv")
    seq_count = whole.shape[0] // groups
    local_heads = query_weight.shape[1]
    unpacked = []
    start = 0
    for weight in weights_list:
        channels = weight.shape[2]
        width = local_heads * channels
        pieces = [
            block[:, start : start + width].reshape(seq_count, local_heads, channels)
            for block in arrived
        ]
        block = jnp.concatenate(pieces, axis=2)
        unpacked.append(block.astype(jnp.float32))
        start = start + width
    query_rows = unpacked[0] * KEY_DIM ** (-0.5)
    key_rows = unpacked[1]
    decay_rows = unpacked[2]
    value_rows = unpacked[3]
    gate_rows = unpacked[4]
    retain = jnp.exp(jax.nn.log_sigmoid(decay_rows + decay_bias) / TAU)
    new_states = retain[..., None] * states + key_rows[..., :, None] * value_rows[..., None, :]
    readout = jnp.einsum("shk,shkv->shv", query_rows, new_states, precision=lax.Precision.HIGHEST)
    readout = (
        readout
        * lax.rsqrt(jnp.mean(readout * readout, axis=-1, keepdims=True) + RMS_EPS)
        * head_gain
    )
    attended = (readout * jax.nn.silu(gate_rows)).astype(jnp.bfloat16)
    seq_count, local_heads, value_width = attended.shape
    flat_width = local_heads * value_width
    halves = lax.axis_size("tp")
    columns = out_weight.shape[1]
    attended = attended.reshape(seq_count, flat_width)
    lanes = jnp.concatenate(gather_blocks(attended, "tp"), axis=1)
    collected = jnp.concatenate(gather_blocks(lanes, "kv"), axis=0)
    mixed_heads = jnp.dot(collected, out_weight, preferred_element_type=jnp.float32)
    residual_own = ALPHA * tokens.astype(jnp.float32) + mixed_heads
    residual_one = gather_columns(residual_own)
    width = residual_one.shape[1]
    average, spread = moments(sums(residual_one), width)
    normed = normalize(residual_one, average, spread, norm_rows[:1], norm_rows[1:])
    lifted = jnp.dot(normed, up_weight, preferred_element_type=jnp.float32)
    hidden = jnp.square(jax.nn.relu(lifted)).astype(jnp.bfloat16)
    mixer_term = jnp.dot(hidden, down_weight, preferred_element_type=jnp.float32)
    rows = mixer_term.shape[0]
    if exchanges("kv") and halves == 2:
        side = lax.axis_index("tp")
        by_side = mixer_term.reshape(rows, groups, halves, columns)
        kept = lax.select(side == 0, by_side[:, :, 0], by_side[:, :, 1])
        given = lax.select(side == 0, by_side[:, :, 1], by_side[:, :, 0])
        half = kept + partner(given, "tp", 1)
        half = half.reshape(rows, groups * columns)
        sent = half.astype(jnp.bfloat16)
        total = half
        for step in range(1, groups):
            total = total + partner(sent, "kv", step).astype(jnp.float32)
        normed_sides = normed.reshape(rows, groups, halves, columns)
        normed_half = lax.select(side == 0, normed_sides[:, :, 0], normed_sides[:, :, 1])
        residual_two = ALPHA * normed_half.reshape(total.shape).astype(jnp.float32) + total
        part = sums(residual_two)
        average, spread = moments(part + partner(part, "tp", 1), width)
        place = lax.axis_index("kv")
    else:
        mixer_all = lax.psum(mixer_term, ("kv", "tp"))
        residual_two = ALPHA * normed.astype(jnp.float32) + mixer_all
        average, spread = moments(sums(residual_two), width)
        place = lax.axis_index(("kv", "tp"))
    own_rows = lax.dynamic_slice_in_dim(residual_two, place * columns, columns, 1)
    layer_out = normalize(own_rows, average, spread, norm2_gain, norm2_bias)
    return (layer_out, new_states)


def solution(mesh):
    placed = (
        P("dp", ("kv", "tp")),
        P(None, "tp", "kv"),
        P(None, "tp", "kv"),
        P(None, "tp", "kv"),
        P(None, "tp", "kv"),
        P(None, "tp", "kv"),
        P("tp", None),
        P(("dp", "kv"), "tp", None, None),
        P("tp", None),
        P(None, ("kv", "tp")),
        P(("kv", "tp")),
        P(("kv", "tp")),
        P(None, ("kv", "tp")),
        P(("kv", "tp"), None),
        P(("kv", "tp")),
        P(("kv", "tp")),
    )
    return jax.shard_map(
        body,
        mesh=mesh,
        in_specs=placed,
        out_specs=(P("dp", ("kv", "tp")), P(("dp", "kv"), "tp", None, None)),
        check_vma=False,
    )
```
